32 devices in a mesh: tp: 4 (over y, x), dp: 8 (over z, core).
Axes of the slice: x: 2, y: 2, z: 4, core: 2. Of those that a mesh axis runs over, the one named last changes fastest.
Arguments:
- stream: bfloat16 [16, 4096], P('tp', 'dp'), may hold values from -48 to 48
- norm_gain: float32 [2, 4096], P(None, 'dp'), may hold values from 0.1 to 1.9
- x_weight: bfloat16 [2, 4096, 8192], P(None, 'dp', 'tp'), may hold values from -0.09375 to 0.09375
- z_weight: bfloat16 [2, 4096, 8192], P(None, 'dp', 'tp'), may hold values from -0.09375 to 0.09375
- bc_weight: bfloat16 [2, 4096, 2, 2048], P(None, 'dp', None, 'tp'), may hold values from -0.09375 to 0.09375
- step_weight: bfloat16 [2, 4096, 128], P(None, 'dp'), may hold values from -0.09375 to 0.09375
- conv_x_weight: bfloat16 [2, 5, 8192], P(None, None, 'tp'), may hold values from -2.5 to 2.5
- conv_bc_weight: bfloat16 [2, 5, 2, 2048], P(None, None, None, 'tp'), may hold values from -2.5 to 2.5
- step_bias: float32 [2, 128], P(None, 'tp'), may hold values from -4 to 0.5
- decay_log: float32 [2, 128], P(None, 'tp'), may hold values from 0 to 2.8
- skip_gain: float32 [2, 128], P(None, 'tp'), may hold values from 0.1 to 1.9
- group_gain: float32 [2, 8192], P(None, 'tp'), may hold values from 0.1 to 1.9
- out_weight: bfloat16 [2, 8192, 4096], P(None, 'tp', 'dp'), may hold values from -0.0625 to 0.0625
- scan_state: float32 [2, 16, 128, 64, 128], P(None, 'dp', 'tp'), may hold values from -1.2 to 1.2
- conv_x_state: bfloat16 [2, 16, 4, 8192], P(None, 'dp', None, 'tp'), may hold values from -6 to 6
- conv_bc_state: bfloat16 [2, 16, 4, 2, 2048], P(None, 'dp', None, None, 'tp'), may hold values from -6 to 6
Outputs:
- stream_out: bfloat16 [16, 4096], P('tp', 'dp')
- scan_state_out: float32 [2, 16, 128, 64, 128], P(None, 'dp', 'tp')
- conv_x_out: bfloat16 [2, 16, 4, 8192], P(None, 'dp', None, 'tp')
- conv_bc_out: bfloat16 [2, 16, 4, 2, 2048], P(None, 'dp', None, None, 'tp')
The draws below stay inside these ranges and needn't reach their ends.
All inputs are finite; a program needn't handle non-finite values.
Results may differ from the reference program's by a relative error of at most 0.04.
Values may be sent and summed in bfloat16 or wider, within the bound.
A program may use at most 64 MiB of HBM per device.

```python
import jax
import jax.numpy as jnp
from jax import lax

MODEL_WIDTH = 4096
HEAD_COUNT = 128
HEAD_DIM = 64
STATE_DIM = 128
GROUPS = 16
KERNEL = 5
LAYERS = 2
SEQUENCES = 16
INNER_WIDTH = 8192
BC_WIDTH = 2048
GROUP_WIDTH = 512
N_DP = 8


def draw_stream(key, part):
    base_key = jax.random.fold_in(key, 11)
    first, second, third = jax.random.split(base_key, 3)
    block_scale = jnp.exp(jax.random.uniform(second, (32,), jnp.float32, jnp.log(0.35), jnp.log(2.8)))
    column_scale = jnp.repeat(block_scale, MODEL_WIDTH // 32)
    values = jnp.clip(jax.random.normal(first, (SEQUENCES, MODEL_WIDTH), jnp.float32), -4.0, 4.0)
    return (values * column_scale[None, :]).astype(jnp.bfloat16)


def shard_levels(stream_key, shape, pieces, least, largest):
    level, own = 1.0, jax.random.fold_in(stream_key, 6)
    for position, shards_of in pieces:
        steps = jnp.exp(jax.random.uniform(jax.random.fold_in(own, position), (shards_of,), jnp.float32, least / len(pieces), largest / len(pieces)))
        level = level * jnp.repeat(steps, shape[position] // shards_of).reshape([-1 if axis == position else 1 for axis in range(len(shape))])
    return level


def gaussian(key, extent, width, bound, cuts=(), kind=jnp.bfloat16):
    entries = width * jax.random.normal(key, extent, jnp.float32)
    if cuts:
        entries = entries * shard_levels(key, extent, cuts, -0.22, 0.18)
    return jnp.clip(entries, -bound, bound).astype(kind)


def setup_inputs(seed: int = 0) -> dict:
    key_of = jax.random.split(jax.random.key(seed), 17)
    return {
        "stream": draw_stream(jax.random.fold_in(key_of[16], 71), 0),
        "norm_gain": jnp.clip(1.0 + 0.18 * jax.random.normal(key_of[1], (LAYERS, MODEL_WIDTH), jnp.float32), 0.1, 1.9),
        "x_weight": gaussian(key_of[2], (LAYERS, MODEL_WIDTH, INNER_WIDTH), MODEL_WIDTH ** -0.5, 0.09375, ((1, 8), (2, 4))),
        "z_weight": gaussian(key_of[3], (LAYERS, MODEL_WIDTH, INNER_WIDTH), MODEL_WIDTH ** -0.5, 0.09375, ((1, 8), (2, 4))),
        "bc_weight": gaussian(key_of[4], (LAYERS, MODEL_WIDTH, 2, BC_WIDTH), MODEL_WIDTH ** -0.5, 0.09375, ((1, 8), (3, 4))),
        "step_weight": gaussian(key_of[5], (LAYERS, MODEL_WIDTH, HEAD_COUNT), MODEL_WIDTH ** -0.5, 0.09375, ((1, 8),)),
        "conv_x_weight": gaussian(key_of[6], (LAYERS, KERNEL, INNER_WIDTH), KERNEL ** -0.5, 2.5, ((2, 4),)),
        "conv_bc_weight": gaussian(key_of[7], (LAYERS, KERNEL, 2, BC_WIDTH), KERNEL ** -0.5, 2.5, ((3, 4),)),
        "step_bias": jnp.clip(-4.0 + 4.5 * jax.random.uniform(key_of[8], (LAYERS, HEAD_COUNT), jnp.float32) ** shard_levels(key_of[8], (LAYERS, HEAD_COUNT), ((1, 4),), -0.2, 0.2), -4.0, 0.5),
        "decay_log": jnp.clip(2.8 * jax.random.uniform(key_of[9], (LAYERS, HEAD_COUNT), jnp.float32) ** shard_levels(key_of[9], (LAYERS, HEAD_COUNT), ((1, 4),), -0.2, 0.2), 0.0, 2.8),
        "skip_gain": jnp.clip(1.0 + 0.18 * jax.random.normal(key_of[10], (LAYERS, HEAD_COUNT), jnp.float32), 0.1, 1.9),
        "group_gain": jnp.clip(1.0 + 0.18 * jax.random.normal(key_of[11], (LAYERS, INNER_WIDTH), jnp.float32), 0.1, 1.9),
        "out_weight": gaussian(key_of[12], (LAYERS, INNER_WIDTH, MODEL_WIDTH), INNER_WIDTH ** -0.5, 0.0625, ((1, 4), (2, 8))),
        "scan_state": gaussian(key_of[13], (LAYERS, SEQUENCES, HEAD_COUNT, HEAD_DIM, STATE_DIM), 0.2, 1.2, ((1, 8), (2, 4)), jnp.float32),
        "conv_x_state": gaussian(key_of[14], (LAYERS, SEQUENCES, KERNEL - 1, INNER_WIDTH), 1.0, 6.0, ((1, 8), (3, 4))),
        "conv_bc_state": gaussian(key_of[15], (LAYERS, SEQUENCES, KERNEL - 1, 2, BC_WIDTH), 1.0, 6.0, ((1, 8), (4, 4))),
    }


EPS = 1e-06

def block_rounded(values):
    rounded = lax.optimization_barrier(values.astype(jnp.bfloat16))
    return lax.optimization_barrier(jnp.sum(rounded.astype(jnp.float32), axis=1))

def split_product(normed_in, weight):
    row_count = normed_in.shape[0]
    columns = weight.shape[1]
    block_rows = MODEL_WIDTH // N_DP
    left = normed_in.astype(jnp.float32).reshape(row_count, N_DP, block_rows)
    right = weight.astype(jnp.float32).reshape(N_DP, block_rows, columns)
    partials = jnp.einsum('skw,kwc->skc', left, right)
    return block_rounded(partials)

def mixer_block(stream, norm_gain, x_weight, z_weight, bc_weight, step_weight, conv_x_weight, conv_bc_weight, step_bias, decay_log, skip_gain, group_gain, out_weight, scan_state, conv_x_state, conv_bc_state):
    row_count = stream.shape[0]
    per_group = HEAD_COUNT // GROUPS
    widened = stream.astype(jnp.float32)
    normed_in = (widened * norm_gain).astype(jnp.bfloat16)
    square_part = lax.optimization_barrier(jnp.sum((widened * widened).reshape(row_count, N_DP, MODEL_WIDTH // N_DP), axis=2))
    inv_rms = lax.rsqrt(block_rounded(square_part)[:, None] / MODEL_WIDTH + EPS)
    proj_x = (split_product(normed_in, x_weight) * inv_rms).astype(jnp.bfloat16)
    proj_z = (split_product(normed_in, z_weight) * inv_rms).astype(jnp.bfloat16)
    proj_bc = (split_product(normed_in, bc_weight.reshape(MODEL_WIDTH, 2 * BC_WIDTH)) * inv_rms).astype(jnp.bfloat16)
    proj_bc = proj_bc.reshape(row_count, 2, BC_WIDTH)
    step_raw = split_product(normed_in, step_weight) * inv_rms
    window_x = jnp.concatenate([conv_x_state, proj_x[:, None, :]], axis=1)
    inputs_x = jax.nn.silu(lax.optimization_barrier(jnp.sum(window_x.astype(jnp.float32) * conv_x_weight.astype(jnp.float32), axis=1)))
    window_bc = jnp.concatenate([conv_bc_state, proj_bc[:, None]], axis=1)
    inputs_bc = jax.nn.silu(lax.optimization_barrier(jnp.sum(window_bc.astype(jnp.float32) * conv_bc_weight.astype(jnp.float32), axis=1)))
    b_part = inputs_bc[:, 0].reshape(row_count, GROUPS, STATE_DIM)
    c_part = inputs_bc[:, 1].reshape(row_count, GROUPS, STATE_DIM)
    step_size = jax.nn.softplus(step_raw + step_bias)
    decay_rate = jnp.exp(-step_size * jnp.exp(decay_log))
    heads_x = inputs_x.reshape(row_count, GROUPS, per_group, HEAD_DIM)
    step_heads = step_size.reshape(row_count, GROUPS, per_group)
    decay_heads = decay_rate.reshape(row_count, GROUPS, per_group)
    old_state = scan_state.reshape(row_count, GROUPS, per_group, HEAD_DIM, STATE_DIM)
    state_new = old_state * decay_heads[..., None, None] + (step_heads[..., None] * heads_x)[..., None] * b_part[:, :, None, None, :]
    readout = jnp.einsum('sgepn,sgn->sgep', state_new, c_part, precision=lax.Precision.HIGHEST)
    readout = readout + skip_gain.reshape(GROUPS, per_group)[None, :, :, None] * heads_x
    gated_out = readout.reshape(row_count, INNER_WIDTH) * jax.nn.silu(proj_z.astype(jnp.float32))
    grouped = gated_out.reshape(row_count, GROUPS, GROUP_WIDTH)
    normed = grouped * lax.rsqrt(lax.optimization_barrier(jnp.mean(grouped * grouped, axis=2, keepdims=True)) + EPS)
    mixed_rows = (normed.reshape(row_count, INNER_WIDTH) * group_gain).astype(jnp.bfloat16)
    update = jnp.dot(mixed_rows, out_weight, preferred_element_type=jnp.float32)
    stream_next = (widened + update).astype(jnp.bfloat16)
    return (stream_next, state_new.reshape(row_count, HEAD_COUNT, HEAD_DIM, STATE_DIM), window_x[:, 1:], window_bc[:, 1:])

def reference(stream, norm_gain, x_weight, z_weight, bc_weight, step_weight, conv_x_weight, conv_bc_weight, step_bias, decay_log, skip_gain, group_gain, out_weight, scan_state, conv_x_state, conv_bc_state):
    current = stream
    states_list = []
    xconv_list = []
    bcconv_list = []
    for block_index in range(LAYERS):
        current, state_next, xconv_next, bcconv_next = mixer_block(current, norm_gain[block_index], x_weight[block_index], z_weight[block_index], bc_weight[block_index], step_weight[block_index], conv_x_weight[block_index], conv_bc_weight[block_index], step_bias[block_index], decay_log[block_index], skip_gain[block_index], group_gain[block_index], out_weight[block_index], scan_state[block_index], conv_x_state[block_index], conv_bc_state[block_index])
        states_list.append(state_next)
        xconv_list.append(xconv_next)
        bcconv_list.append(bcconv_next)
    return (current, jnp.stack(states_list), jnp.stack(xconv_list), jnp.stack(bcconv_list))
```

```python
import functools

import jax
import jax.numpy as jnp
from jax import lax
from jax.experimental import pallas as pl
from jax.experimental.pallas import tpu as pltpu
from jax.sharding import PartitionSpec as P

EPS = 1e-06
LANES = 128
MESH = pl.DeviceIdType.MESH
F32 = jnp.float32
BF16 = jnp.bfloat16


def silu(v):
    return v / (1.0 + jnp.exp(-v))


def expand(rows, hot):
    hi = rows.astype(BF16)
    lo = (rows - hi.astype(F32)).astype(BF16)
    return jnp.dot(hi, hot, preferred_element_type=F32) + jnp.dot(
        lo, hot, preferred_element_type=F32
    )


def kernel(n, t, head_dim, *refs):
    (
        stream, gain, xw, zw, bcw, stw, cxw, cbw, bias, dlog, skip, ggain, ow, st_in, cx_in, cb_in,
        s_out, st_out, cx_out, cb_out,
        v_h, v_gain, v_xw, v_zw, v_bcw, v_stw, v_cxw, v_cbw, v_bias, v_dlog, v_skip, v_ggain, v_ow,
        v_st, v_cx, v_cb, v_cxo, v_cbo, v_so,
        h32, oldbf, hot, consts, pre_x, pre_b, cols, psend, precv, mix, terms, hrow,
        in_sem, h_send, h_recv, p_send, p_recv, m_send, m_recv, t_send, t_recv, out_sem,
    ) = refs
    dp = lax.axis_index("dp")
    tp = lax.axis_index("tp")
    layers, width = v_gain.shape
    X = v_xw.shape[2]
    B = v_bcw.shape[2]
    half = B // 2
    SD = v_st.shape[1]
    groups = half // v_st.shape[3]
    gw = X // groups
    heads = v_bias.shape[1]
    S = h32.shape[0]
    rows = S // t
    taps = v_cxw.shape[1]
    model_width = n * width
    ZO, BO, SO = X, 2 * X, 2 * X + B
    QO = SO + v_stw.shape[2]
    C = QO + LANES

    loads = {}
    count = [0]

    def load(key, src, dst):
        c = pltpu.make_async_copy(src, dst, in_sem.at[count[0]])
        count[0] += 1
        c.start()
        loads[key] = c

    load("h", stream, v_h.at[tp])
    load("gain", gain, v_gain)
    for l in range(layers):
        load(("xw", l), xw.at[l], v_xw.at[l])
        load(("bcw", l), bcw.at[l], v_bcw.at[l])
        load(("stw", l), stw.at[l], v_stw.at[l])
        load(("zw", l), zw.at[l], v_zw.at[l])
        if l == 0:
            load("bias", bias, v_bias)
            load("dlog", dlog, v_dlog)
            load("skip", skip, v_skip)
            load("cxw", cxw, v_cxw)
            load("cbw", cbw, v_cbw)
            load("cx", cx_in, v_cx)
            load("cb", cb_in, v_cb)
            load("ggain", ggain, v_ggain)
        load(("st", l), st_in.at[l], v_st.at[l])
        load(("ow", l), ow.at[l], v_ow.at[l])

    barrier = pltpu.get_barrier_semaphore()
    for k in range(1, t):
        pl.semaphore_signal(barrier, inc=1, device_id={"tp": lax.rem(tp + k, t)}, device_id_type=MESH)
    for k in range(1, n):
        pl.semaphore_signal(barrier, inc=1, device_id={"dp": lax.rem(dp + k, n)}, device_id_type=MESH)
    pl.semaphore_wait(barrier, t + n - 2)

    def push(axis, me, size, k, src, dst, ssem, rsem):
        c = pltpu.make_async_remote_copy(
            src_ref=src, dst_ref=dst, send_sem=ssem, recv_sem=rsem,
            device_id={axis: lax.rem(me + k, size)}, device_id_type=MESH,
        )
        c.start()
        return c

    sent = []
    hc = [
        push("tp", tp, t, k, stream, v_h.at[tp], h_send.at[k], h_recv.at[k]) for k in range(1, t)
    ]
    sent += hc

    kk = lax.broadcasted_iota(jnp.int32, hot.shape, 0) - tp * heads
    cc = lax.broadcasted_iota(jnp.int32, hot.shape, 1)
    low = kk * head_dim
    hot[...] = jnp.where((cc >= low) & (cc < low + head_dim), 1.0, 0.0).astype(BF16)
    k2 = lax.broadcasted_iota(jnp.int32, (heads, X), 0) * head_dim
    c2 = lax.broadcasted_iota(jnp.int32, (heads, X), 1)
    hot2 = jnp.where((c2 >= k2) & (c2 < k2 + head_dim), 1.0, 0.0).astype(BF16)

    loads["h"].wait()
    for c in hc:
        c.wait_recv()
    h32[...] = jnp.concatenate([v_h[i].astype(F32) for i in range(t)], axis=0)
    loads["gain"].wait()

    outs = []
    for l in range(layers):
        hv = h32[...]
        normed = (hv * v_gain[l : l + 1, :]).astype(BF16)
        sq = jnp.sum(hv * hv, axis=1, keepdims=True)

        def project(w_ref, wide, offset):
            step = min(wide, 512)
            for o in range(0, wide, step):
                p = jnp.dot(normed, w_ref[l, :, o : o + step], preferred_element_type=F32)
                p = p.astype(BF16)
                for d in range(n):
                    psend[l, d, :, offset + o : offset + o + step] = p[d * SD : (d + 1) * SD]

        pieces = []

        def scatter(i, lo, hi):
            for k in range(1, n):
                to = lax.rem(dp + k, n)
                pieces.append(
                    push(
                        "dp", dp, n, k,
                        psend.at[l, to, :, lo:hi], precv.at[l, dp, :, lo:hi],
                        p_send.at[l, i, k], p_recv.at[l, i, k],
                    )
                )

        loads["xw", l].wait()
        project(v_xw, X, 0)
        scatter(0, 0, X)
        loads["zw", l].wait()
        project(v_zw, X, ZO)
        scatter(1, ZO, ZO + X)
        loads["bcw", l].wait()
        loads["stw", l].wait()
        project(v_bcw, B, BO)
        project(v_stw, v_stw.shape[2], SO)
        sqb = jnp.broadcast_to(sq, (S, LANES)).astype(BF16)
        for d in range(n):
            psend[l, d, :, QO:C] = sqb[d * SD : (d + 1) * SD]
        scatter(2, BO, C)
        sent += pieces

        if l == 0:
            loads["bias"].wait()
            loads["dlog"].wait()
            loads["skip"].wait()
            stack = jnp.concatenate([v_bias[...], jnp.exp(v_dlog[...]), v_skip[...]], axis=0)
            consts[...] = expand(stack, hot2)
            for key in ("cxw", "cbw", "cx", "cb", "ggain"):
                loads[key].wait()
            for m in range(layers):
                wx = v_cxw[m].astype(F32)[: taps - 1]
                wb = v_cbw[m].astype(F32)[: taps - 1]
                for s in range(SD):
                    pre_x[m, s : s + 1] = jnp.sum(v_cx[m, s].astype(F32) * wx, axis=0, keepdims=True)
                    pre_b[m, s : s + 1] = jnp.sum(v_cb[m, s].astype(F32) * wb, axis=0, keepdims=True)
        loads["st", l].wait()
        for s in range(SD):
            oldbf[s] = v_st[l, s].astype(BF16)

        for c in pieces:
            c.wait_recv()

        def total(lo, hi):
            acc = psend[l, dp, :, lo:hi].astype(F32)
            for k in range(1, n):
                acc = acc + precv[l, lax.rem(dp + k, n), :, lo:hi].astype(F32)
            return acc

        inv = lax.rsqrt(total(QO, C)[:, :1] / model_width + EPS)
        step_raw = total(SO, QO) * inv
        proj_bc = (total(BO, SO) * inv).astype(BF16).astype(F32)
        proj_x = (total(0, X) * inv).astype(BF16).astype(F32)
        proj_z = (total(ZO, ZO + X) * inv).astype(BF16).astype(F32)
        wx = v_cxw[l].astype(F32)[taps - 1 : taps]
        wb = v_cbw[l].astype(F32)[taps - 1 : taps]
        bc = silu(pre_b[l] + proj_bc * wb)
        b = bc[:, :half]
        c = bc[:, half:]
        x = silu(pre_x[l] + proj_x * wx)
        raw = expand(step_raw, hot[...]) + consts[l : l + 1, :]
        step = jnp.maximum(raw, 0.0) + jnp.log1p(jnp.exp(-jnp.abs(raw)))
        decay = jnp.exp(-step * consts[layers + l : layers + l + 1, :])
        dtx = step * x
        cbf = c.astype(BF16)
        gate = silu(proj_z)
        nd = half // groups
        parts = []
        for g in range(groups):
            sl = slice(g * gw, (g + 1) * gw)
            ns = slice(g * nd, (g + 1) * nd)
            picked = []
            for s in range(SD):
                r = lax.dot_general(
                    cbf[:, ns], oldbf[s, sl, :], (((1,), (1,)), ((), ())),
                    preferred_element_type=F32,
                )
                picked.append(r[s : s + 1])
            oldc = jnp.concatenate(picked, axis=0)
            dot_bc = jnp.sum(b[:, ns] * c[:, ns], axis=1, keepdims=True)
            y = (
                decay[:, sl] * oldc
                + dtx[:, sl] * dot_bc
                + consts[2 * layers + l : 2 * layers + l + 1, sl] * x[:, sl]
            )
            y = y * gate[:, sl]
            y = y * lax.rsqrt(jnp.mean(y * y, axis=1, keepdims=True) + EPS)
            parts.append(y * v_ggain[l : l + 1, sl])
        mix[l, dp] = jnp.concatenate(parts, axis=1).astype(BF16)
        mc = [
            push("dp", dp, n, k, mix.at[l, dp], mix.at[l, dp], m_send.at[l, k], m_recv.at[l, k])
            for k in range(1, n)
        ]
        sent += mc

        stack = jnp.concatenate([decay, dtx, decay, dtx], axis=0)[: 4 * SD]
        cols[...] = stack.T
        for s in range(SD):
            for g in range(groups):
                sl = slice(g * gw, (g + 1) * gw)
                brow = b[s : s + 1, g * nd : (g + 1) * nd]
                v_st[l, s, sl, :] = (
                    v_st[l, s, sl, :] * cols[sl, s : s + 1] + cols[sl, SD + s : SD + s + 1] * brow
                )
        oc = pltpu.make_async_copy(v_st.at[l], st_out.at[l], out_sem.at[l])
        oc.start()
        outs.append(oc)
        for s in range(SD):
            v_cxo[l, s] = jnp.concatenate(
                [v_cx[l, s].astype(F32)[1:], proj_x[s : s + 1]], axis=0
            ).astype(BF16)
            v_cbo[l, s] = jnp.concatenate(
                [v_cb[l, s].astype(F32)[1:], proj_bc[s : s + 1]], axis=0
            ).astype(BF16)

        loads["ow", l].wait()
        for cpy in mc:
            cpy.wait_recv()
        allrows = jnp.concatenate([mix[l, d].astype(F32) for d in range(n)], axis=0).astype(BF16)
        terms[l, tp] = jnp.dot(allrows, v_ow[l], preferred_element_type=F32).astype(BF16)
        tc = [
            push("tp", tp, t, k, terms.at[l, tp], terms.at[l, tp], t_send.at[l, k], t_recv.at[l, k])
            for k in range(1, t)
        ]
        sent += tc
        for cpy in tc:
            cpy.wait_recv()
        acc = terms[l, 0].astype(F32)
        for i in range(1, t):
            acc = acc + terms[l, i].astype(F32)
        new = (h32[...] + acc).astype(BF16).astype(F32)
        if l < layers - 1:
            h32[...] = new
        else:
            for i in range(t):
                hrow[i] = new[i * rows : (i + 1) * rows]

    v_so[...] = hrow[tp].astype(BF16)
    for i, (src, dst) in enumerate(((v_so, s_out), (v_cxo, cx_out), (v_cbo, cb_out))):
        oc = pltpu.make_async_copy(src, dst, out_sem.at[layers + i])
        oc.start()
        outs.append(oc)
    for cpy in sent:
        cpy.wait_send()
    for oc in outs:
        oc.wait()


def shards(n, t, *args):
    (
        stream, norm_gain, x_weight, z_weight, bc_weight, step_weight, conv_x_weight,
        conv_bc_weight, step_bias, decay_log, skip_gain, group_gain, out_weight, scan_state,
        conv_x_state, conv_bc_state,
    ) = args
    layers, width = norm_gain.shape
    X = x_weight.shape[2]
    half = bc_weight.shape[3]
    B = 2 * half
    SD, heads, head_dim, sdim = scan_state.shape[1:]
    H = step_weight.shape[2]
    rows = stream.shape[0]
    S = rows * t
    keep = conv_x_state.shape[2]
    taps = conv_x_weight.shape[1]
    bcw = bc_weight.reshape(layers, width, B)
    cbw = conv_bc_weight.reshape(layers, taps, B)
    cbs = conv_bc_state.reshape(layers, SD, keep, B)
    st = scan_state.reshape(layers, SD, heads * head_dim, sdim)
    ins = (
        stream, norm_gain, x_weight, z_weight, bcw, step_weight, conv_x_weight, cbw, step_bias,
        decay_log, skip_gain, group_gain, out_weight, st, conv_x_state, cbs,
    )
    C = 2 * X + B + H + LANES
    dma = pltpu.SemaphoreType.DMA
    V = pltpu.VMEM
    scratch = [V((t, rows, width), BF16)]
    scratch += [V(a.shape, a.dtype) for a in ins[1:]]
    scratch += [
        V(conv_x_state.shape, BF16),
        V(cbs.shape, BF16),
        V(stream.shape, BF16),
        V((S, width), F32),
        V((SD, X, sdim), BF16),
        V((H, X), BF16),
        V((3 * layers, X), F32),
        V((layers, SD, X), F32),
        V((layers, SD, B), F32),
        V((X, 4 * SD), F32),
        V((layers, n, SD, C), BF16),
        V((layers, n, SD, C), BF16),
        V((layers, n, SD, X), BF16),
        V((layers, t, S, out_weight.shape[2]), BF16),
        V((t, rows, width), F32),
        dma((10 + 6 * layers,)),
        dma((t,)),
        dma((t,)),
        dma((layers, 3, n)),
        dma((layers, 3, n)),
        dma((layers, n)),
        dma((layers, n)),
        dma((layers, t)),
        dma((layers, t)),
        dma((layers + 3,)),
    ]
    any_spec = pl.BlockSpec(memory_space=pl.ANY)
    res = pl.pallas_call(
        functools.partial(kernel, n, t, head_dim),
        out_shape=(
            jax.ShapeDtypeStruct(stream.shape, BF16),
            jax.ShapeDtypeStruct(st.shape, F32),
            jax.ShapeDtypeStruct(conv_x_state.shape, BF16),
            jax.ShapeDtypeStruct(cbs.shape, BF16),
        ),
        in_specs=[any_spec] * len(ins),
        out_specs=[any_spec] * 4,
        scratch_shapes=scratch,
        compiler_params=pltpu.CompilerParams(
            collective_id=0, has_side_effects=True, vmem_limit_bytes=60 * 1024 * 1024
        ),
        name="mixers",
    )(*ins)
    return (
        res[0], res[1].reshape(scan_state.shape), res[2], res[3].reshape(conv_bc_state.shape)
    )


def solution(mesh):
    n, t = mesh.shape["dp"], mesh.shape["tp"]
    in_specs = (
        P("tp", "dp"),
        P(None, "dp"),
        P(None, "dp", "tp"),
        P(None, "dp", "tp"),
        P(None, "dp", None, "tp"),
        P(None, "dp", None),
        P(None, None, "tp"),
        P(None, None, None, "tp"),
        P(None, "tp"),
        P(None, "tp"),
        P(None, "tp"),
        P(None, "tp"),
        P(None, "tp", "dp"),
        P(None, "dp", "tp", None, None),
        P(None, "dp", None, "tp"),
        P(None, "dp", None, None, "tp"),
    )
    out_specs = (
        P("tp", "dp"),
        P(None, "dp", "tp", None, None),
        P(None, "dp", None, "tp"),
        P(None, "dp", None, None, "tp"),
    )
    return jax.shard_map(
        functools.partial(shards, n, t),
        mesh=mesh, in_specs=in_specs, out_specs=out_specs, check_vma=False,
    )
```

```python
import functools

import jax
import jax.numpy as jnp
from jax import lax
from jax.experimental import pallas as pl
from jax.experimental.pallas import tpu as pltpu
from jax.sharding import PartitionSpec as P

EPS = 1e-06
LANES = 128
VMEM_GRANT = 56 * 1024 * 1024
MESH = pl.DeviceIdType.MESH
F32 = jnp.float32
BF16 = jnp.bfloat16


def silu(v):
    return v / (1.0 + jnp.exp(-v))


def expand(rows, hot):
    hi = rows.astype(BF16)
    lo = (rows - hi.astype(F32)).astype(BF16)
    return jnp.dot(hi, hot, preferred_element_type=F32) + jnp.dot(
        lo, hot, preferred_element_type=F32
    )


def kernel(n, t, head_dim, *refs):
    (
        stream, gain, xw, zw, bcw, stw, cxw, cbw, bias, dlog, skip, ggain, ow, st_in, cx_in, cb_in,
        v_so, v_st, v_cxo, v_cbo,
        v_h, v_gain, v_xw, v_zw, v_bcw, v_stw, v_cxw, v_cbw, v_bias, v_dlog, v_skip, v_ggain, v_ow,
        v_cx, v_cb,
        h32, oldbf, hot, spread, consts, pre_x, pre_b, cols, psend, precv, mix, terms, hrow,
        in_sem, h_send, h_recv, p_send, p_recv, m_send, m_recv, t_send, t_recv,
    ) = refs
    dp = lax.axis_index("dp")
    tp = lax.axis_index("tp")
    layers, width = v_gain.shape
    X = v_xw.shape[2]
    half = v_cb.shape[4]
    B = 2 * half
    tiles = v_bcw.shape[1]
    SD = v_st.shape[1]
    groups = half // v_st.shape[3]
    gw = X // groups
    heads = v_bias.shape[1]
    S = h32.shape[0]
    rows = S // t
    taps = v_cxw.shape[0]
    model_width = n * width
    ZO, BO, SO = X, 2 * X, 2 * X + B
    QO = SO + v_stw.shape[2]
    C = QO + LANES

    loads = {}
    count = [0]

    def load(key, src, dst):
        c = pltpu.make_async_copy(src, dst, in_sem.at[count[0]])
        count[0] += 1
        c.start()
        loads[key] = c

    load("h", stream, v_h.at[tp])
    load("gain", gain, v_gain)
    for l in range(layers):
        load(("xw", l), xw.at[l], v_xw.at[l])
        for j in range(tiles):
            load(("bcw", l, j), bcw.at[l, :, :, j * LANES : (j + 1) * LANES], v_bcw.at[l, j])
        load(("stw", l), stw.at[l], v_stw.at[l])
        load(("zw", l), zw.at[l], v_zw.at[l])
        if l == 0:
            load("bias", bias, v_bias)
            load("dlog", dlog, v_dlog)
            load("skip", skip, v_skip)
            load("cxw", cxw, v_cxw)
            load("cbw", cbw, v_cbw)
            load("cx", cx_in, v_cx)
            load("cb", cb_in, v_cb)
            load("ggain", ggain, v_ggain)
        load(("st", l), st_in.at[l], v_st.at[l])
        load(("ow", l), ow.at[l], v_ow.at[l])

    barrier = pltpu.get_barrier_semaphore()
    for k in range(1, t):
        pl.semaphore_signal(barrier, inc=1, device_id={"tp": lax.rem(tp + k, t)}, device_id_type=MESH)
    for k in range(1, n):
        pl.semaphore_signal(barrier, inc=1, device_id={"dp": lax.rem(dp + k, n)}, device_id_type=MESH)
    pl.semaphore_wait(barrier, t + n - 2)

    def push(axis, me, size, k, src, dst, ssem, rsem):
        c = pltpu.make_async_remote_copy(
            src_ref=src, dst_ref=dst, send_sem=ssem, recv_sem=rsem,
            device_id={axis: lax.rem(me + k, size)}, device_id_type=MESH,
        )
        c.start()
        return c

    sent = []
    hc = [
        push("tp", tp, t, k, stream, v_h.at[tp], h_send.at[k], h_recv.at[k]) for k in range(1, t)
    ]
    sent += hc

    kk = lax.broadcasted_iota(jnp.int32, hot.shape, 0) - tp * heads
    cc = lax.broadcasted_iota(jnp.int32, hot.shape, 1)
    low = kk * head_dim
    hot[...] = jnp.where((cc >= low) & (cc < low + head_dim), 1.0, 0.0).astype(BF16)
    k2 = lax.broadcasted_iota(jnp.int32, (heads, X), 0) * head_dim
    c2 = lax.broadcasted_iota(jnp.int32, (heads, X), 1)
    hot2 = jnp.where((c2 >= k2) & (c2 < k2 + head_dim), 1.0, 0.0).astype(BF16)

    i3 = lax.broadcasted_iota(jnp.int32, spread.shape, 0) * 2
    c3 = lax.broadcasted_iota(jnp.int32, spread.shape, 1)
    spread[...] = jnp.where(i3 == c3, 1.0, 0.0).astype(BF16)

    loads["h"].wait()
    for c in hc:
        c.wait_recv()
    h32[...] = jnp.concatenate([v_h[i].astype(F32) for i in range(t)], axis=0)
    loads["gain"].wait()

    for l in range(layers):
        hv = h32[...]
        normed = (hv * v_gain[l : l + 1, :]).astype(BF16)
        sq = jnp.sum(hv * hv, axis=1, keepdims=True)

        def project(w_ref, wide, offset):
            step = min(wide, 512)
            for o in range(0, wide, step):
                p = jnp.dot(normed, w_ref[l, :, o : o + step], preferred_element_type=F32)
                p = p.astype(BF16)
                for d in range(n):
                    psend[l, d, :, offset + o : offset + o + step] = p[d * SD : (d + 1) * SD]

        pieces = []

        def scatter(i, lo, hi):
            for k in range(1, n):
                to = lax.rem(dp + k, n)
                pieces.append(
                    push(
                        "dp", dp, n, k,
                        psend.at[l, to, :, lo:hi], precv.at[l, dp, :, lo:hi],
                        p_send.at[l, i, k], p_recv.at[l, i, k],
                    )
                )

        loads["xw", l].wait()
        project(v_xw, X, 0)
        scatter(0, 0, X)
        loads["zw", l].wait()
        project(v_zw, X, ZO)
        scatter(1, ZO, ZO + X)
        even = jnp.dot(normed, spread[...], preferred_element_type=F32)
        both = jnp.concatenate([even, pltpu.roll(even, 1, 1)], axis=0).astype(BF16)
        for j in range(tiles):
            loads["bcw", l, j].wait()
            w = v_bcw.at[l, j].reshape(2 * width, LANES)[...]
            p = jnp.dot(both, w, preferred_element_type=F32).astype(BF16)
            for d in range(n):
                o = BO + j * LANES
                psend[l, d, :, o : o + LANES] = p[d * SD : (d + 1) * SD]
                psend[l, d, :, o + half : o + half + LANES] = p[S + d * SD : S + (d + 1) * SD]
        loads["stw", l].wait()
        project(v_stw, v_stw.shape[2], SO)
        sqb = jnp.broadcast_to(sq, (S, LANES)).astype(BF16)
        for d in range(n):
            psend[l, d, :, QO:C] = sqb[d * SD : (d + 1) * SD]
        scatter(2, BO, C)
        sent += pieces

        if l == 0:
            loads["bias"].wait()
            loads["dlog"].wait()
            loads["skip"].wait()
            stack = jnp.concatenate([v_bias[...], jnp.exp(v_dlog[...]), v_skip[...]], axis=0)
            consts[...] = expand(stack, hot2)
            for key in ("cxw", "cbw", "cx", "cb", "ggain"):
                loads[key].wait()
            for m in range(layers):
                wxs = [v_cxw[k].astype(F32)[m : m + 1] for k in range(taps)]
                for s in range(SD):
                    old = v_cx[m, s].astype(F32)
                    pre_x[m, s : s + 1] = sum(old[k : k + 1] * wxs[k] for k in range(taps - 1))
                    both = sum(
                        v_cb[m, s, k].astype(F32) * v_cbw[m, k].astype(F32) for k in range(taps - 1)
                    )
                    pre_b[m, s : s + 1] = jnp.concatenate([both[:1], both[1:]], axis=1)
        loads["st", l].wait()
        for s in range(SD):
            oldbf[s] = v_st[l, s].astype(BF16)

        for c in pieces:
            c.wait_recv()

        def total(lo, hi):
            acc = psend[l, dp, :, lo:hi].astype(F32)
            for k in range(1, n):
                acc = acc + precv[l, lax.rem(dp + k, n), :, lo:hi].astype(F32)
            return acc

        inv = lax.rsqrt(total(QO, C)[:, :1] / model_width + EPS)
        step_raw = total(SO, QO) * inv
        proj_bc = (total(BO, SO) * inv).astype(BF16).astype(F32)
        proj_x = (total(0, X) * inv).astype(BF16).astype(F32)
        proj_z = (total(ZO, ZO + X) * inv).astype(BF16).astype(F32)
        wx = v_cxw[taps - 1].astype(F32)[l : l + 1]
        wb = v_cbw[l, taps - 1].astype(F32)
        wb = jnp.concatenate([wb[:1], wb[1:]], axis=1)
        bc = silu(pre_b[l] + proj_bc * wb)
        b = bc[:, :half]
        c = bc[:, half:]
        x = silu(pre_x[l] + proj_x * wx)
        raw = expand(step_raw, hot[...]) + consts[l : l + 1, :]
        step = jnp.maximum(raw, 0.0) + jnp.log1p(jnp.exp(-jnp.abs(raw)))
        decay = jnp.exp(-step * consts[layers + l : layers + l + 1, :])
        dtx = step * x
        cbf = c.astype(BF16)
        gate = silu(proj_z)
        nd = half // groups
        parts = []
        for g in range(groups):
            sl = slice(g * gw, (g + 1) * gw)
            ns = slice(g * nd, (g + 1) * nd)
            picked = []
            for s in range(SD):
                r = lax.dot_general(
                    cbf[:, ns], oldbf[s, sl, :], (((1,), (1,)), ((), ())),
                    preferred_element_type=F32,
                )
                picked.append(r[s : s + 1])
            oldc = jnp.concatenate(picked, axis=0)
            dot_bc = jnp.sum(b[:, ns] * c[:, ns], axis=1, keepdims=True)
            y = (
                decay[:, sl] * oldc
                + dtx[:, sl] * dot_bc
                + consts[2 * layers + l : 2 * layers + l + 1, sl] * x[:, sl]
            )
            y = y * gate[:, sl]
            y = y * lax.rsqrt(jnp.mean(y * y, axis=1, keepdims=True) + EPS)
            parts.append(y * v_ggain[l : l + 1, sl])
        mix[l, dp] = jnp.concatenate(parts, axis=1).astype(BF16)
        mc = [
            push("dp", dp, n, k, mix.at[l, dp], mix.at[l, dp], m_send.at[l, k], m_recv.at[l, k])
            for k in range(1, n)
        ]
        sent += mc

        stack = jnp.concatenate([decay, dtx, decay, dtx], axis=0)[: 4 * SD]
        cols[...] = stack.T
        for s in range(SD):
            for g in range(groups):
                sl = slice(g * gw, (g + 1) * gw)
                brow = b[s : s + 1, g * nd : (g + 1) * nd]
                v_st[l, s, sl, :] = (
                    v_st[l, s, sl, :] * cols[sl, s : s + 1] + cols[sl, SD + s : SD + s + 1] * brow
                )
        for s in range(SD):
            v_cxo[l, s] = jnp.concatenate(
                [v_cx[l, s].astype(F32)[1:], proj_x[s : s + 1]], axis=0
            ).astype(BF16)
            for k in range(taps - 2):
                v_cbo[l, s, k] = v_cb[l, s, k + 1]
            v_cbo[l, s, taps - 2] = jnp.concatenate(
                [proj_bc[s : s + 1, :half], proj_bc[s : s + 1, half:]], axis=0
            ).astype(BF16)

        loads["ow", l].wait()
        for cpy in mc:
            cpy.wait_recv()
        allrows = jnp.concatenate([mix[l, d].astype(F32) for d in range(n)], axis=0).astype(BF16)
        terms[l, tp] = jnp.dot(allrows, v_ow[l], preferred_element_type=F32).astype(BF16)
        tc = [
            push("tp", tp, t, k, terms.at[l, tp], terms.at[l, tp], t_send.at[l, k], t_recv.at[l, k])
            for k in range(1, t)
        ]
        sent += tc
        for cpy in tc:
            cpy.wait_recv()
        acc = terms[l, 0].astype(F32)
        for i in range(1, t):
            acc = acc + terms[l, i].astype(F32)
        new = (h32[...] + acc).astype(BF16).astype(F32)
        if l < layers - 1:
            h32[...] = new
        else:
            for i in range(t):
                hrow[i] = new[i * rows : (i + 1) * rows]

    v_so[...] = hrow[tp].astype(BF16)
    for cpy in sent:
        cpy.wait_send()


def store(*refs):
    sem = refs[-1]
    half = (len(refs) - 1) // 2
    copies = [pltpu.make_async_copy(refs[i], refs[half + i], sem.at[i]) for i in range(half)]
    for c in copies:
        c.start()
    for c in copies:
        c.wait()


def shards(n, t, *args):
    (
        stream, norm_gain, x_weight, z_weight, bc_weight, step_weight, conv_x_weight,
        conv_bc_weight, step_bias, decay_log, skip_gain, group_gain, out_weight, scan_state,
        conv_x_state, conv_bc_state,
    ) = args
    layers, width = norm_gain.shape
    X = x_weight.shape[2]
    half = bc_weight.shape[3]
    B = 2 * half
    SD, heads, head_dim, sdim = scan_state.shape[1:]
    H = step_weight.shape[2]
    rows = stream.shape[0]
    S = rows * t
    keep = conv_x_state.shape[2]
    taps = conv_x_weight.shape[1]
    cxw = jnp.transpose(conv_x_weight, (1, 0, 2))
    st = scan_state.reshape(layers, SD, heads * head_dim, sdim)
    ins = (
        stream, norm_gain, x_weight, z_weight, bc_weight, step_weight, cxw, conv_bc_weight, step_bias,
        decay_log, skip_gain, group_gain, out_weight, st, conv_x_state, conv_bc_state,
    )
    C = 2 * X + B + H + LANES
    dma = pltpu.SemaphoreType.DMA
    V = pltpu.VMEM
    scratch = [V((t, rows, width), BF16)]
    shapes = [a.shape for a in ins]
    shapes[4] = (layers, half // LANES, width, 2, LANES)
    scratch += [V(shapes[i], ins[i].dtype) for i in range(1, len(ins)) if i != 13]
    scratch += [
        V((S, width), F32),
        V((SD, X, sdim), BF16),
        V((H, X), BF16),
        V((width, 2 * width), BF16),
        V((3 * layers, X), F32),
        V((layers, SD, X), F32),
        V((layers, SD, B), F32),
        V((X, 4 * SD), F32),
        V((layers, n, SD, C), BF16),
        V((layers, n, SD, C), BF16),
        V((layers, n, SD, X), BF16),
        V((layers, t, S, out_weight.shape[2]), BF16),
        V((t, rows, width), F32),
        dma((10 + (5 + half // LANES) * layers,)),
        dma((t,)),
        dma((t,)),
        dma((layers, 3, n)),
        dma((layers, 3, n)),
        dma((layers, n)),
        dma((layers, n)),
        dma((layers, t)),
        dma((layers, t)),
    ]
    any_spec = pl.BlockSpec(memory_space=pl.ANY)
    vmem_spec = pl.BlockSpec(memory_space=V)
    outs = (stream, st, conv_x_state, conv_bc_state)
    res = pl.pallas_call(
        functools.partial(kernel, n, t, head_dim),
        out_shape=tuple(V(a.shape, a.dtype) for a in outs),
        in_specs=[any_spec] * len(ins),
        out_specs=[vmem_spec] * len(outs),
        scratch_shapes=scratch,
        compiler_params=pltpu.CompilerParams(
            collective_id=0, has_side_effects=True, vmem_limit_bytes=VMEM_GRANT
        ),
        name="mixers",
    )(*ins)
    res = [pltpu.with_memory_space_constraint(r, V) for r in res]
    res = pl.pallas_call(
        store,
        out_shape=tuple(jax.ShapeDtypeStruct(a.shape, a.dtype) for a in outs),
        in_specs=[vmem_spec] * len(outs),
        out_specs=[any_spec] * len(outs),
        scratch_shapes=[dma((len(outs),))],
        compiler_params=pltpu.CompilerParams(vmem_limit_bytes=VMEM_GRANT),
        name="store",
    )(*res)
    return (res[0], res[1].reshape(scan_state.shape), res[2], res[3])


def solution(mesh):
    n, t = mesh.shape["dp"], mesh.shape["tp"]
    in_specs = (
        P("tp", "dp"),
        P(None, "dp"),
        P(None, "dp", "tp"),
        P(None, "dp", "tp"),
        P(None, "dp", None, "tp"),
        P(None, "dp", None),
        P(None, None, "tp"),
        P(None, None, None, "tp"),
        P(None, "tp"),
        P(None, "tp"),
        P(None, "tp"),
        P(None, "tp"),
        P(None, "tp", "dp"),
        P(None, "dp", "tp", None, None),
        P(None, "dp", None, "tp"),
        P(None, "dp", None, None, "tp"),
    )
    out_specs = (
        P("tp", "dp"),
        P(None, "dp", "tp", None, None),
        P(None, "dp", None, "tp"),
        P(None, "dp", None, None, "tp"),
    )
    return jax.shard_map(
        functools.partial(shards, n, t),
        mesh=mesh, in_specs=in_specs, out_specs=out_specs, check_vma=False,
    )
```

```python
import functools

import jax
import jax.numpy as jnp
from jax import lax
from jax.experimental import pallas as pl
from jax.experimental.pallas import tpu as pltpu
from jax.sharding import PartitionSpec as P

EPS = 1e-06
LANES = 128
VMEM_GRANT = 56 * 1024 * 1024
MESH = pl.DeviceIdType.MESH
F32 = jnp.float32
BF16 = jnp.bfloat16


def silu(v):
    return v / (1.0 + jnp.exp(-v))


def expand(rows, hot):
    hi = rows.astype(BF16)
    lo = (rows - hi.astype(F32)).astype(BF16)
    return jnp.dot(hi, hot, preferred_element_type=F32) + jnp.dot(
        lo, hot, preferred_element_type=F32
    )


def kernel(n, t, head_dim, *refs):
    (
        stream, gain, xw, zw, bcw, stw, cxw, cbw, bias, dlog, skip, ggain, ow, st_in, cx_in, cb_in,
        v_so, v_st, v_cxo, v_cbo,
        v_h, v_gain, v_xw, v_zw, v_bcw, v_stw, v_cxw, v_cbw, v_bias, v_dlog, v_skip, v_ggain, v_ow,
        v_cx, v_cb,
        h32, oldbf, hot, spread, consts, pre_x, pre_b, cols, psend, precv, mix, terms, hrow, lsend, lrecv,
        in_sem, h_send, h_recv, p_send, p_recv, m_send, m_recv, t_send, t_recv,
    ) = refs
    dp = lax.axis_index("dp")
    tp = lax.axis_index("tp")
    layers, width = v_gain.shape
    X = v_xw.shape[2]
    half = v_cb.shape[4]
    B = 2 * half
    tiles = v_bcw.shape[1]
    SD = v_st.shape[1]
    groups = half // v_st.shape[3]
    gw = X // groups
    heads = v_bias.shape[1]
    S = h32.shape[0]
    rows = S // t
    taps = v_cxw.shape[0]
    model_width = n * width
    ZO, BO, SO = X, 2 * X, 2 * X + B
    QO = SO + v_stw.shape[2]
    C = QO + LANES

    loads = {}
    count = [0]

    def load(key, src, dst):
        c = pltpu.make_async_copy(src, dst, in_sem.at[count[0]])
        count[0] += 1
        c.start()
        loads[key] = c

    load("h", stream, v_h.at[tp])
    load("gain", gain, v_gain)
    for l in range(layers):
        load(("xw", l), xw.at[l], v_xw.at[l])
        for j in range(tiles):
            load(("bcw", l, j), bcw.at[l, :, :, j * LANES : (j + 1) * LANES], v_bcw.at[l, j])
        load(("stw", l), stw.at[l], v_stw.at[l])
        load(("zw", l), zw.at[l], v_zw.at[l])
        if l == 0:
            load("bias", bias, v_bias)
            load("dlog", dlog, v_dlog)
            load("skip", skip, v_skip)
            load("cxw", cxw, v_cxw)
            load("cbw", cbw, v_cbw)
            load("cx", cx_in, v_cx)
            load("cb", cb_in, v_cb)
            load("ggain", ggain, v_ggain)
        load(("st", l), st_in.at[l], v_st.at[l])
        load(("ow", l), ow.at[l], v_ow.at[l])

    barrier = pltpu.get_barrier_semaphore()
    for k in range(1, t):
        pl.semaphore_signal(barrier, inc=1, device_id={"tp": lax.rem(tp + k, t)}, device_id_type=MESH)
    for k in range(1, n):
        pl.semaphore_signal(barrier, inc=1, device_id={"dp": lax.rem(dp + k, n)}, device_id_type=MESH)
    pl.semaphore_wait(barrier, t + n - 2)

    def push(axis, me, size, k, src, dst, ssem, rsem):
        c = pltpu.make_async_remote_copy(
            src_ref=src, dst_ref=dst, send_sem=ssem, recv_sem=rsem,
            device_id={axis: lax.rem(me + k, size)}, device_id_type=MESH,
        )
        c.start()
        return c

    side = dp // max(n // 2, 1)

    def peer(j):
        up, down = n - 1 - j, j
        far_up = up - 1 + (up + n - dp - 1) // n
        far_down = down + 1 - (dp - down - 1 + n) // n
        return side * far_down + (1 - side) * far_up

    def along(src, dst, ssem, rsem):
        made = []
        for j in range(n - 1):
            to = peer(j)
            c = pltpu.make_async_remote_copy(
                src_ref=src(to), dst_ref=dst(dp), send_sem=ssem(j), recv_sem=rsem(dp),
                device_id={"dp": to}, device_id_type=MESH,
            )
            c.start()
            made.append(c)
        waits = []
        for k in range(1, n):
            come = lax.rem(dp + k, n)
            waits.append(
                pltpu.make_async_remote_copy(
                    src_ref=src(come), dst_ref=dst(come), send_sem=ssem(0), recv_sem=rsem(come),
                    device_id={"dp": come}, device_id_type=MESH,
                )
            )
        sent.extend(made)
        return waits

    sent = []
    hc = [
        push("tp", tp, t, k, stream, v_h.at[tp], h_send.at[k], h_recv.at[k]) for k in range(1, t)
    ]
    sent += hc

    kk = lax.broadcasted_iota(jnp.int32, hot.shape, 0) - tp * heads
    cc = lax.broadcasted_iota(jnp.int32, hot.shape, 1)
    low = kk * head_dim
    hot[...] = jnp.where((cc >= low) & (cc < low + head_dim), 1.0, 0.0).astype(BF16)
    k2 = lax.broadcasted_iota(jnp.int32, (heads, X), 0) * head_dim
    c2 = lax.broadcasted_iota(jnp.int32, (heads, X), 1)
    hot2 = jnp.where((c2 >= k2) & (c2 < k2 + head_dim), 1.0, 0.0).astype(BF16)

    i3 = lax.broadcasted_iota(jnp.int32, spread.shape, 0) * 2
    c3 = lax.broadcasted_iota(jnp.int32, spread.shape, 1)
    spread[...] = jnp.where(i3 == c3, 1.0, 0.0).astype(BF16)

    loads["h"].wait()
    for c in hc:
        c.wait_recv()
    h32[...] = jnp.concatenate([v_h[i].astype(F32) for i in range(t)], axis=0)
    loads["gain"].wait()

    for l in range(layers):
        hv = h32[...]
        normed = (hv * v_gain[l : l + 1, :]).astype(BF16)
        sq = jnp.sum(hv * hv, axis=1, keepdims=True)

        def project(w_ref, wide, offset):
            step = min(wide, 512)
            for o in range(0, wide, step):
                p = jnp.dot(normed, w_ref[l, :, o : o + step], preferred_element_type=F32)
                p = p.astype(BF16)
                for d in range(n):
                    psend[l, d, :, offset + o : offset + o + step] = p[d * SD : (d + 1) * SD]

        pieces = []

        def scatter(i, lo, hi):
            pieces.extend(
                along(
                    lambda d: psend.at[l, d, :, lo:hi], lambda d: precv.at[l, d, :, lo:hi],
                    lambda j: p_send.at[l, i, j], lambda d: p_recv.at[l, i, d],
                )
            )

        loads["xw", l].wait()
        project(v_xw, X, 0)
        scatter(0, 0, X)
        loads["zw", l].wait()
        project(v_zw, X, ZO)
        scatter(1, ZO, ZO + X)
        even = jnp.dot(normed, spread[...], preferred_element_type=F32)
        both = jnp.concatenate([even, pltpu.roll(even, 1, 1)], axis=0).astype(BF16)
        for j in range(tiles):
            loads["bcw", l, j].wait()
            w = v_bcw.at[l, j].reshape(2 * width, LANES)[...]
            p = jnp.dot(both, w, preferred_element_type=F32).astype(BF16)
            for d in range(n):
                o = BO + j * LANES
                psend[l, d, :, o : o + LANES] = p[d * SD : (d + 1) * SD]
                psend[l, d, :, o + half : o + half + LANES] = p[S + d * SD : S + (d + 1) * SD]
        loads["stw", l].wait()
        project(v_stw, v_stw.shape[2], SO)
        sqb = jnp.broadcast_to(sq, (S, LANES)).astype(BF16)
        for d in range(n):
            psend[l, d, :, QO:C] = sqb[d * SD : (d + 1) * SD]
        scatter(2, BO, C)

        if l == 0:
            loads["bias"].wait()
            loads["dlog"].wait()
            loads["skip"].wait()
            stack = jnp.concatenate([v_bias[...], jnp.exp(v_dlog[...]), v_skip[...]], axis=0)
            consts[...] = expand(stack, hot2)
            for key in ("cxw", "cbw", "cx", "cb", "ggain"):
                loads[key].wait()
            for m in range(layers):
                wxs = [v_cxw[k].astype(F32)[m : m + 1] for k in range(taps)]
                for s in range(SD):
                    old = v_cx[m, s].astype(F32)
                    pre_x[m, s : s + 1] = sum(old[k : k + 1] * wxs[k] for k in range(taps - 1))
                    both = sum(
                        v_cb[m, s, k].astype(F32) * v_cbw[m, k].astype(F32) for k in range(taps - 1)
                    )
                    pre_b[m, s : s + 1] = jnp.concatenate([both[:1], both[1:]], axis=1)
        loads["st", l].wait()
        for s in range(SD):
            oldbf[s] = v_st[l, s].astype(BF16)

        for c in pieces:
            c.wait_recv()

        def total(lo, hi):
            acc = psend[l, dp, :, lo:hi].astype(F32)
            for k in range(1, n):
                acc = acc + precv[l, lax.rem(dp + k, n), :, lo:hi].astype(F32)
            return acc

        inv = lax.rsqrt(total(QO, C)[:, :1] / model_width + EPS)
        step_raw = total(SO, QO) * inv
        proj_bc = (total(BO, SO) * inv).astype(BF16).astype(F32)
        proj_x = (total(0, X) * inv).astype(BF16).astype(F32)
        proj_z = (total(ZO, ZO + X) * inv).astype(BF16).astype(F32)
        wx = v_cxw[taps - 1].astype(F32)[l : l + 1]
        wb = v_cbw[l, taps - 1].astype(F32)
        wb = jnp.concatenate([wb[:1], wb[1:]], axis=1)
        bc = silu(pre_b[l] + proj_bc * wb)
        b = bc[:, :half]
        c = bc[:, half:]
        x = silu(pre_x[l] + proj_x * wx)
        raw = expand(step_raw, hot[...]) + consts[l : l + 1, :]
        step = jnp.maximum(raw, 0.0) + jnp.log1p(jnp.exp(-jnp.abs(raw)))
        decay = jnp.exp(-step * consts[layers + l : layers + l + 1, :])
        dtx = step * x
        cbf = c.astype(BF16)
        gate = silu(proj_z)
        nd = half // groups
        parts = []
        for g in range(groups):
            sl = slice(g * gw, (g + 1) * gw)
            ns = slice(g * nd, (g + 1) * nd)
            picked = []
            for s in range(SD):
                r = lax.dot_general(
                    cbf[:, ns], oldbf[s, sl, :], (((1,), (1,)), ((), ())),
                    preferred_element_type=F32,
                )
                picked.append(r[s : s + 1])
            oldc = jnp.concatenate(picked, axis=0)
            dot_bc = jnp.sum(b[:, ns] * c[:, ns], axis=1, keepdims=True)
            y = (
                decay[:, sl] * oldc
                + dtx[:, sl] * dot_bc
                + consts[2 * layers + l : 2 * layers + l + 1, sl] * x[:, sl]
            )
            y = y * gate[:, sl]
            y = y * lax.rsqrt(jnp.mean(y * y, axis=1, keepdims=True) + EPS)
            parts.append(y * v_ggain[l : l + 1, sl])
        mix[l, dp] = jnp.concatenate(parts, axis=1).astype(BF16)
        mc = along(
            lambda d: mix.at[l, dp], lambda d: mix.at[l, d],
            lambda j: m_send.at[l, j], lambda d: m_recv.at[l, d],
        )

        stack = jnp.concatenate([decay, dtx, decay, dtx], axis=0)[: 4 * SD]
        cols[...] = stack.T
        for s in range(SD):
            for g in range(groups):
                sl = slice(g * gw, (g + 1) * gw)
                brow = b[s : s + 1, g * nd : (g + 1) * nd]
                v_st[l, s, sl, :] = (
                    v_st[l, s, sl, :] * cols[sl, s : s + 1] + cols[sl, SD + s : SD + s + 1] * brow
                )
        for s in range(SD):
            v_cxo[l, s] = jnp.concatenate(
                [v_cx[l, s].astype(F32)[1:], proj_x[s : s + 1]], axis=0
            ).astype(BF16)
            for k in range(taps - 2):
                v_cbo[l, s, k] = v_cb[l, s, k + 1]
            v_cbo[l, s, taps - 2] = jnp.concatenate(
                [proj_bc[s : s + 1, :half], proj_bc[s : s + 1, half:]], axis=0
            ).astype(BF16)

        loads["ow", l].wait()
        for cpy in mc:
            cpy.wait_recv()
        allrows = jnp.concatenate([mix[l, d].astype(F32) for d in range(n)], axis=0).astype(BF16)
        term = jnp.dot(allrows, v_ow[l], preferred_element_type=F32).astype(BF16)
        last = l == layers - 1
        if last:
            for i in range(t):
                lsend[i] = term[i * rows : (i + 1) * rows]
        else:
            terms[l, tp] = term
        tc = []
        for k in range(1, t):
            src = lsend.at[lax.rem(tp + k, t)] if last else terms.at[l, tp]
            dst = lrecv.at[tp] if last else terms.at[l, tp]
            tc.append(push("tp", tp, t, k, src, dst, t_send.at[l, k], t_recv.at[l, k]))
        sent += tc
        if last:
            for i in range(t):
                hrow[i] = h32[i * rows : (i + 1) * rows]
            acc = lsend[tp].astype(F32)
        for cpy in tc:
            cpy.wait_recv()
        if last:
            for k in range(1, t):
                acc = acc + lrecv[lax.rem(tp + k, t)].astype(F32)
            v_so[...] = (hrow[tp] + acc).astype(BF16)
        else:
            acc = terms[l, 0].astype(F32)
            for i in range(1, t):
                acc = acc + terms[l, i].astype(F32)
            h32[...] = (h32[...] + acc).astype(BF16).astype(F32)

    for cpy in sent:
        cpy.wait_send()


def store(*refs):
    sem = refs[-1]
    half = (len(refs) - 1) // 2
    copies = [pltpu.make_async_copy(refs[i], refs[half + i], sem.at[i]) for i in range(half)]
    for c in copies:
        c.start()
    for c in copies:
        c.wait()


def shards(n, t, *args):
    (
        stream, norm_gain, x_weight, z_weight, bc_weight, step_weight, conv_x_weight,
        conv_bc_weight, step_bias, decay_log, skip_gain, group_gain, out_weight, scan_state,
        conv_x_state, conv_bc_state,
    ) = args
    layers, width = norm_gain.shape
    X = x_weight.shape[2]
    half = bc_weight.shape[3]
    B = 2 * half
    SD, heads, head_dim, sdim = scan_state.shape[1:]
    H = step_weight.shape[2]
    rows = stream.shape[0]
    S = rows * t
    keep = conv_x_state.shape[2]
    taps = conv_x_weight.shape[1]
    cxw = jnp.transpose(conv_x_weight, (1, 0, 2))
    st = scan_state.reshape(layers, SD, heads * head_dim, sdim)
    ins = (
        stream, norm_gain, x_weight, z_weight, bc_weight, step_weight, cxw, conv_bc_weight, step_bias,
        decay_log, skip_gain, group_gain, out_weight, st, conv_x_state, conv_bc_state,
    )
    C = 2 * X + B + H + LANES
    dma = pltpu.SemaphoreType.DMA
    V = pltpu.VMEM
    scratch = [V((t, rows, width), BF16)]
    shapes = [a.shape for a in ins]
    shapes[4] = (layers, half // LANES, width, 2, LANES)
    scratch += [V(shapes[i], ins[i].dtype) for i in range(1, len(ins)) if i != 13]
    scratch += [
        V((S, width), F32),
        V((SD, X, sdim), BF16),
        V((H, X), BF16),
        V((width, 2 * width), BF16),
        V((3 * layers, X), F32),
        V((layers, SD, X), F32),
        V((layers, SD, B), F32),
        V((X, 4 * SD), F32),
        V((layers, n, SD, C), BF16),
        V((layers, n, SD, C), BF16),
        V((layers, n, SD, X), BF16),
        V((layers, t, S, out_weight.shape[2]), BF16),
        V((t, rows, width), F32),
        V((t, rows, width), BF16),
        V((t, rows, width), BF16),
        dma((10 + (5 + half // LANES) * layers,)),
        dma((t,)),
        dma((t,)),
        dma((layers, 3, n)),
        dma((layers, 3, n)),
        dma((layers, n)),
        dma((layers, n)),
        dma((layers, t)),
        dma((layers, t)),
    ]
    any_spec = pl.BlockSpec(memory_space=pl.ANY)
    vmem_spec = pl.BlockSpec(memory_space=V)
    outs = (stream, st, conv_x_state, conv_bc_state)
    res = pl.pallas_call(
        functools.partial(kernel, n, t, head_dim),
        out_shape=tuple(V(a.shape, a.dtype) for a in outs),
        in_specs=[any_spec] * len(ins),
        out_specs=[vmem_spec] * len(outs),
        scratch_shapes=scratch,
        compiler_params=pltpu.CompilerParams(
            collective_id=0, has_side_effects=True, vmem_limit_bytes=VMEM_GRANT
        ),
        name="mixers",
    )(*ins)
    res = [pltpu.with_memory_space_constraint(r, V) for r in res]
    res = pl.pallas_call(
        store,
        out_shape=tuple(jax.ShapeDtypeStruct(a.shape, a.dtype) for a in outs),
        in_specs=[vmem_spec] * len(outs),
        out_specs=[any_spec] * len(outs),
        scratch_shapes=[dma((len(outs),))],
        compiler_params=pltpu.CompilerParams(vmem_limit_bytes=VMEM_GRANT),
        name="store",
    )(*res)
    return (res[0], res[1].reshape(scan_state.shape), res[2], res[3])


def solution(mesh):
    n, t = mesh.shape["dp"], mesh.shape["tp"]
    in_specs = (
        P("tp", "dp"),
        P(None, "dp"),
        P(None, "dp", "tp"),
        P(None, "dp", "tp"),
        P(None, "dp", None, "tp"),
        P(None, "dp", None),
        P(None, None, "tp"),
        P(None, None, None, "tp"),
        P(None, "tp"),
        P(None, "tp"),
        P(None, "tp"),
        P(None, "tp"),
        P(None, "tp", "dp"),
        P(None, "dp", "tp", None, None),
        P(None, "dp", None, "tp"),
        P(None, "dp", None, None, "tp"),
    )
    out_specs = (
        P("tp", "dp"),
        P(None, "dp", "tp", None, None),
        P(None, "dp", None, "tp"),
        P(None, "dp", None, None, "tp"),
    )
    return jax.shard_map(
        functools.partial(shards, n, t),
        mesh=mesh, in_specs=in_specs, out_specs=out_specs, check_vma=False,
    )
```

```python
import functools

import jax
import jax.numpy as jnp
from jax import lax
from jax.experimental import pallas as pl
from jax.experimental.pallas import tpu as pltpu
from jax.sharding import PartitionSpec as P

EPS = 1e-06
LANES = 128
VMEM_GRANT = 56 * 1024 * 1024
MESH = pl.DeviceIdType.MESH
F32 = jnp.float32
BF16 = jnp.bfloat16


def silu(v):
    return v / (1.0 + jnp.exp(-v))


def expand(rows, hot):
    hi = rows.astype(BF16)
    lo = (rows - hi.astype(F32)).astype(BF16)
    return jnp.dot(hi, hot, preferred_element_type=F32) + jnp.dot(
        lo, hot, preferred_element_type=F32
    )


def kernel(n, t, head_dim, *refs):
    (
        stream, gain, xw, zw, bcw, stw, cxw, cbw, bias, dlog, skip, ggain, ow, st_in, cx_in, cb_in,
        v_so, v_st, v_cxo, v_cbo,
        v_h, v_gain, v_xw, v_zw, v_bcw, v_stw, v_cxw, v_cbw, v_bias, v_dlog, v_skip, v_ggain, v_ow,
        v_cx, v_cb,
        h32, oldbf, hot, spread, consts, pre_x, pre_b, cols, psend, precv, mix, terms, hrow, lsend, lrecv,
        in_sem, h_send, h_recv, p_send, p_recv, m_send, m_recv, t_send, t_recv,
    ) = refs
    dp = lax.axis_index("dp")
    tp = lax.axis_index("tp")
    layers, width = v_gain.shape
    X = v_xw.shape[2]
    half = v_cb.shape[4]
    B = 2 * half
    tiles = v_bcw.shape[1]
    SD = v_st.shape[1]
    groups = half // v_st.shape[3]
    gw = X // groups
    heads = v_bias.shape[1]
    S = h32.shape[0]
    rows = S // t
    taps = v_cxw.shape[0]
    model_width = n * width
    ZO, BO, SO = X, 2 * X, 2 * X + B
    QO = SO + v_stw.shape[2]
    C = QO + LANES

    loads = {}
    count = [0]

    def load(key, src, dst):
        c = pltpu.make_async_copy(src, dst, in_sem.at[count[0]])
        count[0] += 1
        c.start()
        loads[key] = c

    load("h", stream, v_h.at[tp])
    load("gain", gain, v_gain)
    for l in range(layers):
        load(("xw", l), xw.at[l], v_xw.at[l])
        load(("zw", l), zw.at[l], v_zw.at[l])
        for j in range(tiles):
            load(("bcw", l, j), bcw.at[l, :, :, j * LANES : (j + 1) * LANES], v_bcw.at[l, j])
        load(("stw", l), stw.at[l], v_stw.at[l])
        if l == 0:
            load("bias", bias, v_bias)
            load("dlog", dlog, v_dlog)
            load("skip", skip, v_skip)
            load("cxw", cxw, v_cxw)
            load("cbw", cbw, v_cbw)
            load("cx", cx_in, v_cx)
            load("cb", cb_in, v_cb)
            load("ggain", ggain, v_ggain)
        load(("st", l), st_in.at[l], v_st.at[l])
        load(("ow", l), ow.at[l], v_ow.at[l])

    barrier = pltpu.get_barrier_semaphore()
    for k in range(1, t):
        pl.semaphore_signal(barrier, inc=1, device_id={"tp": lax.rem(tp + k, t)}, device_id_type=MESH)
    for k in range(1, n):
        pl.semaphore_signal(barrier, inc=1, device_id={"dp": lax.rem(dp + k, n)}, device_id_type=MESH)
    pl.semaphore_wait(barrier, t + n - 2)

    def push(axis, me, size, k, src, dst, ssem, rsem):
        c = pltpu.make_async_remote_copy(
            src_ref=src, dst_ref=dst, send_sem=ssem, recv_sem=rsem,
            device_id={axis: lax.rem(me + k, size)}, device_id_type=MESH,
        )
        c.start()
        return c

    side = dp // max(n // 2, 1)

    def peer(j):
        up, down = n - 1 - j, j
        far_up = up - 1 + (up + n - dp - 1) // n
        far_down = down + 1 - (dp - down - 1 + n) // n
        return side * far_down + (1 - side) * far_up

    def along(src, dst, ssem, rsem):
        made = []
        for j in range(n - 1):
            to = peer(j)
            c = pltpu.make_async_remote_copy(
                src_ref=src(to), dst_ref=dst(dp), send_sem=ssem(j), recv_sem=rsem(dp),
                device_id={"dp": to}, device_id_type=MESH,
            )
            c.start()
            made.append(c)
        waits = []
        for k in range(1, n):
            come = lax.rem(dp + k, n)
            waits.append(
                pltpu.make_async_remote_copy(
                    src_ref=src(come), dst_ref=dst(come), send_sem=ssem(0), recv_sem=rsem(come),
                    device_id={"dp": come}, device_id_type=MESH,
                )
            )
        sent.extend(made)
        return waits

    sent = []
    hc = [
        push("tp", tp, t, k, stream, v_h.at[tp], h_send.at[k], h_recv.at[k]) for k in range(1, t)
    ]
    sent += hc

    kk = lax.broadcasted_iota(jnp.int32, hot.shape, 0) - tp * heads
    cc = lax.broadcasted_iota(jnp.int32, hot.shape, 1)
    low = kk * head_dim
    hot[...] = jnp.where((cc >= low) & (cc < low + head_dim), 1.0, 0.0).astype(BF16)
    k2 = lax.broadcasted_iota(jnp.int32, (heads, X), 0) * head_dim
    c2 = lax.broadcasted_iota(jnp.int32, (heads, X), 1)
    hot2 = jnp.where((c2 >= k2) & (c2 < k2 + head_dim), 1.0, 0.0).astype(BF16)

    i3 = lax.broadcasted_iota(jnp.int32, spread.shape, 0) * 2
    c3 = lax.broadcasted_iota(jnp.int32, spread.shape, 1)
    spread[...] = jnp.where(i3 == c3, 1.0, 0.0).astype(BF16)

    loads["h"].wait()
    for c in hc:
        c.wait_recv()
    h32[...] = jnp.concatenate([v_h[i].astype(F32) for i in range(t)], axis=0)
    loads["gain"].wait()

    for l in range(layers):
        hv = h32[...]
        normed = (hv * v_gain[l : l + 1, :]).astype(BF16)
        sq = jnp.sum(hv * hv, axis=1, keepdims=True)

        def project(w_ref, wide, offset):
            step = min(wide, 512)
            for o in range(0, wide, step):
                p = jnp.dot(normed, w_ref[l, :, o : o + step], preferred_element_type=F32)
                p = p.astype(BF16)
                for d in range(n):
                    psend[l, d, :, offset + o : offset + o + step] = p[d * SD : (d + 1) * SD]

        pieces = []

        def scatter(i, lo, hi):
            pieces.extend(
                along(
                    lambda d: psend.at[l, d, :, lo:hi], lambda d: precv.at[l, d, :, lo:hi],
                    lambda j: p_send.at[l, i, j], lambda d: p_recv.at[l, i, d],
                )
            )

        loads["xw", l].wait()
        project(v_xw, X, 0)
        scatter(0, 0, X)
        loads["zw", l].wait()
        project(v_zw, X, ZO)
        scatter(1, ZO, ZO + X)
        even = jnp.dot(normed, spread[...], preferred_element_type=F32)
        both = jnp.concatenate([even, pltpu.roll(even, 1, 1)], axis=0).astype(BF16)
        for j in range(tiles):
            loads["bcw", l, j].wait()
            w = v_bcw.at[l, j].reshape(2 * width, LANES)[...]
            p = jnp.dot(both, w, preferred_element_type=F32).astype(BF16)
            for d in range(n):
                o = BO + j * LANES
                psend[l, d, :, o : o + LANES] = p[d * SD : (d + 1) * SD]
                psend[l, d, :, o + half : o + half + LANES] = p[S + d * SD : S + (d + 1) * SD]
        loads["stw", l].wait()
        project(v_stw, v_stw.shape[2], SO)
        sqb = jnp.broadcast_to(sq, (S, LANES)).astype(BF16)
        for d in range(n):
            psend[l, d, :, QO:C] = sqb[d * SD : (d + 1) * SD]
        scatter(2, BO, C)

        if l == 0:
            loads["bias"].wait()
            loads["dlog"].wait()
            loads["skip"].wait()
            stack = jnp.concatenate([v_bias[...], jnp.exp(v_dlog[...]), v_skip[...]], axis=0)
            consts[...] = expand(stack, hot2)
            for key in ("cxw", "cbw", "cx", "cb", "ggain"):
                loads[key].wait()
            for m in range(layers):
                wxs = [v_cxw[k].astype(F32)[m : m + 1] for k in range(taps)]
                for s in range(SD):
                    old = v_cx[m, s].astype(F32)
                    pre_x[m, s : s + 1] = sum(old[k : k + 1] * wxs[k] for k in range(taps - 1))
                    both = sum(
                        v_cb[m, s, k].astype(F32) * v_cbw[m, k].astype(F32) for k in range(taps - 1)
                    )
                    pre_b[m, s : s + 1] = jnp.concatenate([both[:1], both[1:]], axis=1)
        loads["st", l].wait()
        for s in range(SD):
            oldbf[s] = v_st[l, s].astype(BF16)

        def total(lo, hi):
            acc = psend[l, dp, :, lo:hi].astype(F32)
            for k in range(1, n):
                acc = acc + precv[l, lax.rem(dp + k, n), :, lo:hi].astype(F32)
            return acc

        for c in pieces[: n - 1]:
            c.wait_recv()
        sum_x = total(0, X)
        for c in pieces[n - 1 : 2 * (n - 1)]:
            c.wait_recv()
        sum_z = total(ZO, ZO + X)
        for c in pieces[2 * (n - 1) :]:
            c.wait_recv()
        inv = lax.rsqrt(total(QO, C)[:, :1] / model_width + EPS)
        step_raw = total(SO, QO) * inv
        proj_bc = (total(BO, SO) * inv).astype(BF16).astype(F32)
        proj_x = (sum_x * inv).astype(BF16).astype(F32)
        proj_z = (sum_z * inv).astype(BF16).astype(F32)
        wx = v_cxw[taps - 1].astype(F32)[l : l + 1]
        wb = v_cbw[l, taps - 1].astype(F32)
        wb = jnp.concatenate([wb[:1], wb[1:]], axis=1)
        bc = silu(pre_b[l] + proj_bc * wb)
        b = bc[:, :half]
        c = bc[:, half:]
        x = silu(pre_x[l] + proj_x * wx)
        raw = expand(step_raw, hot[...]) + consts[l : l + 1, :]
        step = jnp.maximum(raw, 0.0) + jnp.log1p(jnp.exp(-jnp.abs(raw)))
        decay = jnp.exp(-step * consts[layers + l : layers + l + 1, :])
        dtx = step * x
        cbf = c.astype(BF16)
        gate = silu(proj_z)
        nd = half // groups
        parts = []
        for g in range(groups):
            sl = slice(g * gw, (g + 1) * gw)
            ns = slice(g * nd, (g + 1) * nd)
            picked = []
            for s in range(SD):
                r = lax.dot_general(
                    cbf[:, ns], oldbf[s, sl, :], (((1,), (1,)), ((), ())),
                    preferred_element_type=F32,
                )
                picked.append(r[s : s + 1])
            oldc = jnp.concatenate(picked, axis=0)
            dot_bc = jnp.sum(b[:, ns] * c[:, ns], axis=1, keepdims=True)
            y = (
                decay[:, sl] * oldc
                + dtx[:, sl] * dot_bc
                + consts[2 * layers + l : 2 * layers + l + 1, sl] * x[:, sl]
            )
            y = y * gate[:, sl]
            y = y * lax.rsqrt(jnp.mean(y * y, axis=1, keepdims=True) + EPS)
            parts.append(y * v_ggain[l : l + 1, sl])
        mix[l, dp] = jnp.concatenate(parts, axis=1).astype(BF16)
        mc = along(
            lambda d: mix.at[l, dp], lambda d: mix.at[l, d],
            lambda j: m_send.at[l, j], lambda d: m_recv.at[l, d],
        )

        stack = jnp.concatenate([decay, dtx, decay, dtx], axis=0)[: 4 * SD]
        cols[...] = stack.T
        for s in range(SD):
            for g in range(groups):
                sl = slice(g * gw, (g + 1) * gw)
                brow = b[s : s + 1, g * nd : (g + 1) * nd]
                v_st[l, s, sl, :] = (
                    v_st[l, s, sl, :] * cols[sl, s : s + 1] + cols[sl, SD + s : SD + s + 1] * brow
                )
        for s in range(SD):
            v_cxo[l, s] = jnp.concatenate(
                [v_cx[l, s].astype(F32)[1:], proj_x[s : s + 1]], axis=0
            ).astype(BF16)
            for k in range(taps - 2):
                v_cbo[l, s, k] = v_cb[l, s, k + 1]
            v_cbo[l, s, taps - 2] = jnp.concatenate(
                [proj_bc[s : s + 1, :half], proj_bc[s : s + 1, half:]], axis=0
            ).astype(BF16)

        loads["ow", l].wait()
        for cpy in mc:
            cpy.wait_recv()
        allrows = jnp.concatenate([mix[l, d].astype(F32) for d in range(n)], axis=0).astype(BF16)
        term = jnp.dot(allrows, v_ow[l], preferred_element_type=F32).astype(BF16)
        last = l == layers - 1
        if last:
            for i in range(t):
                lsend[i] = term[i * rows : (i + 1) * rows]
        else:
            terms[l, tp] = term
        tc = []
        for k in range(1, t):
            src = lsend.at[lax.rem(tp + k, t)] if last else terms.at[l, tp]
            dst = lrecv.at[tp] if last else terms.at[l, tp]
            tc.append(push("tp", tp, t, k, src, dst, t_send.at[l, k], t_recv.at[l, k]))
        sent += tc
        if last:
            for i in range(t):
                hrow[i] = h32[i * rows : (i + 1) * rows]
            acc = lsend[tp].astype(F32)
        for cpy in tc:
            cpy.wait_recv()
        if last:
            for k in range(1, t):
                acc = acc + lrecv[lax.rem(tp + k, t)].astype(F32)
            v_so[...] = (hrow[tp] + acc).astype(BF16)
        else:
            acc = terms[l, 0].astype(F32)
            for i in range(1, t):
                acc = acc + terms[l, i].astype(F32)
            h32[...] = (h32[...] + acc).astype(BF16).astype(F32)

    for cpy in sent:
        cpy.wait_send()


def store(*refs):
    sem = refs[-1]
    half = (len(refs) - 1) // 2
    copies = [pltpu.make_async_copy(refs[i], refs[half + i], sem.at[i]) for i in range(half)]
    for c in copies:
        c.start()
    for c in copies:
        c.wait()


def shards(n, t, *args):
    (
        stream, norm_gain, x_weight, z_weight, bc_weight, step_weight, conv_x_weight,
        conv_bc_weight, step_bias, decay_log, skip_gain, group_gain, out_weight, scan_state,
        conv_x_state, conv_bc_state,
    ) = args
    layers, width = norm_gain.shape
    X = x_weight.shape[2]
    half = bc_weight.shape[3]
    B = 2 * half
    SD, heads, head_dim, sdim = scan_state.shape[1:]
    H = step_weight.shape[2]
    rows = stream.shape[0]
    S = rows * t
    keep = conv_x_state.shape[2]
    taps = conv_x_weight.shape[1]
    cxw = jnp.transpose(conv_x_weight, (1, 0, 2))
    st = scan_state.reshape(layers, SD, heads * head_dim, sdim)
    ins = (
        stream, norm_gain, x_weight, z_weight, bc_weight, step_weight, cxw, conv_bc_weight, step_bias,
        decay_log, skip_gain, group_gain, out_weight, st, conv_x_state, conv_bc_state,
    )
    C = 2 * X + B + H + LANES
    dma = pltpu.SemaphoreType.DMA
    V = pltpu.VMEM
    scratch = [V((t, rows, width), BF16)]
    shapes = [a.shape for a in ins]
    shapes[4] = (layers, half // LANES, width, 2, LANES)
    scratch += [V(shapes[i], ins[i].dtype) for i in range(1, len(ins)) if i != 13]
    scratch += [
        V((S, width), F32),
        V((SD, X, sdim), BF16),
        V((H, X), BF16),
        V((width, 2 * width), BF16),
        V((3 * layers, X), F32),
        V((layers, SD, X), F32),
        V((layers, SD, B), F32),
        V((X, 4 * SD), F32),
        V((layers, n, SD, C), BF16),
        V((layers, n, SD, C), BF16),
        V((layers, n, SD, X), BF16),
        V((layers, t, S, out_weight.shape[2]), BF16),
        V((t, rows, width), F32),
        V((t, rows, width), BF16),
        V((t, rows, width), BF16),
        dma((10 + (5 + half // LANES) * layers,)),
        dma((t,)),
        dma((t,)),
        dma((layers, 3, n)),
        dma((layers, 3, n)),
        dma((layers, n)),
        dma((layers, n)),
        dma((layers, t)),
        dma((layers, t)),
    ]
    any_spec = pl.BlockSpec(memory_space=pl.ANY)
    vmem_spec = pl.BlockSpec(memory_space=V)
    outs = (stream, st, conv_x_state, conv_bc_state)
    res = pl.pallas_call(
        functools.partial(kernel, n, t, head_dim),
        out_shape=tuple(V(a.shape, a.dtype) for a in outs),
        in_specs=[any_spec] * len(ins),
        out_specs=[vmem_spec] * len(outs),
        scratch_shapes=scratch,
        compiler_params=pltpu.CompilerParams(
            collective_id=0, has_side_effects=True, vmem_limit_bytes=VMEM_GRANT
        ),
        name="mixers",
    )(*ins)
    res = [pltpu.with_memory_space_constraint(r, V) for r in res]
    res = pl.pallas_call(
        store,
        out_shape=tuple(jax.ShapeDtypeStruct(a.shape, a.dtype) for a in outs),
        in_specs=[vmem_spec] * len(outs),
        out_specs=[any_spec] * len(outs),
        scratch_shapes=[dma((len(outs),))],
        compiler_params=pltpu.CompilerParams(vmem_limit_bytes=VMEM_GRANT),
        name="store",
    )(*res)
    return (res[0], res[1].reshape(scan_state.shape), res[2], res[3])


def solution(mesh):
    n, t = mesh.shape["dp"], mesh.shape["tp"]
    in_specs = (
        P("tp", "dp"),
        P(None, "dp"),
        P(None, "dp", "tp"),
        P(None, "dp", "tp"),
        P(None, "dp", None, "tp"),
        P(None, "dp", None),
        P(None, None, "tp"),
        P(None, None, None, "tp"),
        P(None, "tp"),
        P(None, "tp"),
        P(None, "tp"),
        P(None, "tp"),
        P(None, "tp", "dp"),
        P(None, "dp", "tp", None, None),
        P(None, "dp", None, "tp"),
        P(None, "dp", None, None, "tp"),
    )
    out_specs = (
        P("tp", "dp"),
        P(None, "dp", "tp", None, None),
        P(None, "dp", None, "tp"),
        P(None, "dp", None, None, "tp"),
    )
    return jax.shard_map(
        functools.partial(shards, n, t),
        mesh=mesh, in_specs=in_specs, out_specs=out_specs, check_vma=False,
    )
```
